32 devices in a mesh: sp: 4 (over z), tp: 8 (over y, x, core).
Axes of the slice: x: 2, y: 2, z: 4, core: 2. Of those that a mesh axis runs over, the one named last changes fastest.
Arguments:
- latent: bfloat16 [2048, 4096], P(('sp', 'tp')), may hold values from -6 to 6
- context: bfloat16 [512, 4096], P('sp'), may hold values from -6 to 6
- condition: float32 [4096], P('sp'), may hold values from -6 to 6
- context_cond: float32 [4096], P('sp'), may hold values from -6 to 6
- mod_weight: bfloat16 [4096, 12288], P('sp', 'tp'), may hold values from -0.09375 to 0.09375
- norm_gain: float32 [4096], replicated, may hold values from 0.1 to 1.9
- query_weight: bfloat16 [4096, 4096], P(None, 'tp'), may hold values from -0.09375 to 0.09375
- key_weight: bfloat16 [4096, 2048], P(None, 'tp'), may hold values from -0.09375 to 0.09375
- value_weight: bfloat16 [4096, 2048], P(None, 'tp'), may hold values from -0.09375 to 0.09375
- out_weight: bfloat16 [4096, 4096], P(None, 'tp'), may hold values from -0.375 to 0.375
- query_gain: float32 [64], replicated, may hold values from 1.2 to 6
- key_gain: float32 [64], replicated, may hold values from 1.2 to 6
- context_lift: float32 [64], P('tp'), may hold values from 0.5 to 2
Outputs:
- updated: bfloat16 [2048, 4096], P(('sp', 'tp'))
The draws below stay inside these ranges and needn't reach their ends.
All inputs are finite; a program needn't handle non-finite values.
Results may differ from the reference program's by a relative error of at most 0.0085.
The reference program's roundings to bfloat16 on the way count: a program that leaves them out, or rounds other values in their place, can miss the bound.
Values may be sent and summed in bfloat16 or wider, within the bound.
A program may use at most 64 MiB of HBM per device.

```python
import math
import jax
import jax.numpy as jnp
from jax import lax

D = 4096
HD = 64
Q_HEADS = 64
KV_HEADS = 32
GRID_W = 64
CTX = 512
SEQ = 2048


def draw_query_gain(key, part):
    subkey = jax.random.fold_in(key, 101)
    return jax.random.uniform(subkey, (HD,), jnp.float32, 1.2, 2.0)


def draw_key_gain(key, part):
    subkey = jax.random.fold_in(key, 202)
    return jax.random.uniform(subkey, (HD,), jnp.float32, 1.2, 2.0)


def block_scale(rng, dims, split, low, largest):
    level, own = 1.0, jax.random.fold_in(rng, 6)
    for position, shards_of in split:
        draws = jnp.exp(jax.random.uniform(jax.random.fold_in(own, position), (shards_of,), jnp.float32, low / len(split), largest / len(split)))
        level = level * jnp.repeat(draws, dims[position] // shards_of).reshape([-1 if axis == position else 1 for axis in range(len(dims))])
    return level


def normal_values(rng, dims, spread, reach, pieces=(), kind=jnp.bfloat16):
    result = spread * jax.random.normal(rng, dims, jnp.float32)
    if pieces:
        result = result * block_scale(rng, dims, pieces, -0.22, 0.18)
    return jnp.clip(result, -reach, reach).astype(kind)


def setup_inputs(seed: int = 0) -> dict:
    seeds = jax.random.split(jax.random.key(seed), 14)
    latent = normal_values(seeds[0], (SEQ, D), 1.0, 6.0, ((0, 32),))
    context = normal_values(seeds[1], (CTX, D), 1.0, 6.0, ((0, 4),))
    condition = normal_values(seeds[2], (D,), 1.0, 6.0, ((0, 4),), jnp.float32)
    context_cond = normal_values(seeds[3], (D,), 1.0, 6.0, ((0, 4),), jnp.float32)
    mod_weight = normal_values(seeds[4], (D, 3 * D), D ** -0.5, 0.09375, ((0, 4), (1, 8)))
    norm_gain = jnp.clip(1.0 + 0.18 * jax.random.normal(seeds[5], (D,), jnp.float32), 0.1, 1.9)
    query_weight = normal_values(seeds[6], (D, Q_HEADS * HD), D ** -0.5, 0.09375, ((1, 8),))
    key_weight = normal_values(seeds[7], (D, KV_HEADS * HD), D ** -0.5, 0.09375, ((1, 8),))
    value_weight = normal_values(seeds[8], (D, KV_HEADS * HD), D ** -0.5, 0.09375, ((1, 8),))
    out_weight = normal_values(seeds[9], (Q_HEADS * HD, D), (Q_HEADS * HD // 16) ** -0.5, 0.375, ((1, 8),))
    query_gain = draw_query_gain(jax.random.fold_in(seeds[13], 71), 0)
    key_gain = draw_key_gain(jax.random.fold_in(seeds[13], 71), 0)
    context_lift = jnp.clip(0.5 + 1.5 * jax.random.uniform(seeds[12], (Q_HEADS,), jnp.float32) ** block_scale(seeds[12], (Q_HEADS,), ((0, 8),), -0.2, 0.2), 0.5, 2.0)
    return {"latent": latent, "context": context, "condition": condition, "context_cond": context_cond, "mod_weight": mod_weight, "norm_gain": norm_gain, "query_weight": query_weight, "key_weight": key_weight, "value_weight": value_weight, "out_weight": out_weight, "query_gain": query_gain, "key_gain": key_gain, "context_lift": context_lift}


EPS = 1e-06

def modulate(row_block, gain_vec, mod_row, model_width):
    row_values = row_block.astype(jnp.float32)
    normal = row_values * lax.rsqrt(lax.optimization_barrier(jnp.mean(row_values * row_values, axis=-1, keepdims=True)) + EPS)
    shift_part = mod_row[:model_width]
    scale_part = mod_row[model_width:2 * model_width]
    return (normal * gain_vec * (1.0 + scale_part) + shift_part).astype(jnp.bfloat16)

def head_norm(values, gain_vec):
    return values * lax.rsqrt(lax.optimization_barrier(jnp.mean(values * values, axis=-1, keepdims=True)) + EPS) * gain_vec

def rope_tables(positions, head_size):
    freq_count = head_size // 4
    inverse = 10000.0 ** (-jnp.arange(freq_count, dtype=jnp.float32) / freq_count)
    grid_row = (positions // GRID_W).astype(jnp.float32)
    grid_col = (positions % GRID_W).astype(jnp.float32)
    angles = jnp.concatenate([grid_row[:, None] * inverse, grid_col[:, None] * inverse], axis=-1)
    return (jnp.cos(angles), jnp.sin(angles))

def rotate(values, cos_table, sin_table):
    paired = values.reshape(values.shape[:-1] + (values.shape[-1] // 2, 2))
    even_part = paired[..., 0]
    odd_part = paired[..., 1]
    cos_wide = cos_table[:, None, :]
    sin_wide = sin_table[:, None, :]
    turned = jnp.stack([even_part * cos_wide - odd_part * sin_wide, even_part * sin_wide + odd_part * cos_wide], axis=-1)
    return turned.reshape(values.shape)

def reference(latent, context, condition, context_cond, mod_weight, norm_gain, query_weight, key_weight, value_weight, out_weight, query_gain, key_gain, context_lift):
    model_width = latent.shape[1]
    cond_pair = jax.nn.silu(jnp.stack([condition, context_cond]).astype(jnp.float32)).astype(jnp.bfloat16)
    modulation = jnp.dot(cond_pair, mod_weight, preferred_element_type=jnp.float32)
    normed = modulate(latent, norm_gain, modulation[0], model_width)
    normed_ctx = modulate(context, norm_gain, modulation[1], model_width)
    positions = jnp.arange(SEQ, dtype=jnp.int32)
    cos_table, sin_table = rope_tables(positions, HD)
    query_raw = jnp.dot(normed, query_weight, preferred_element_type=jnp.float32).reshape(SEQ, Q_HEADS, HD)
    queries = rotate(head_norm(query_raw, query_gain), cos_table, sin_table).astype(jnp.bfloat16)
    key_raw = jnp.dot(normed, key_weight, preferred_element_type=jnp.float32).reshape(SEQ, KV_HEADS, HD)
    keys = rotate(head_norm(key_raw, key_gain), cos_table, sin_table).astype(jnp.bfloat16)
    values = jnp.dot(normed, value_weight, preferred_element_type=jnp.float32).astype(jnp.bfloat16)
    ctx_raw = jnp.dot(normed_ctx, key_weight, preferred_element_type=jnp.float32).reshape(CTX, KV_HEADS, HD)
    ctx_keys = head_norm(ctx_raw, key_gain).astype(jnp.bfloat16)
    ctx_values = jnp.dot(normed_ctx, value_weight, preferred_element_type=jnp.float32).astype(jnp.bfloat16)
    group_size = Q_HEADS // KV_HEADS
    score_scale = HD ** (-0.5)
    query_heads = queries.reshape(SEQ, KV_HEADS, group_size, HD).transpose(1, 0, 2, 3)
    key_heads = keys.transpose(1, 0, 2)
    value_heads = values.reshape(SEQ, KV_HEADS, HD).transpose(1, 0, 2)
    ctx_key_heads = ctx_keys.transpose(1, 0, 2)
    ctx_value_heads = ctx_values.reshape(CTX, KV_HEADS, HD).transpose(1, 0, 2)
    lift_rows = context_lift.reshape(KV_HEADS, group_size)
    query_block = math.gcd(SEQ, 512)

    def per_head(inputs):
        q_head, k_head, v_head, ck_head, cv_head, lift_row = inputs
        k_wide = k_head.astype(jnp.float32)
        v_wide = v_head.astype(jnp.float32)
        ck_wide = ck_head.astype(jnp.float32)
        cv_wide = cv_head.astype(jnp.float32)
        blocks = q_head.reshape(SEQ // query_block, query_block, group_size, HD)

        def per_block(q_block):
            q_wide = q_block.astype(jnp.float32)
            lat_scores = jnp.einsum('qgd,kd->gqk', q_wide, k_wide) * score_scale
            ctx_scores = jnp.einsum('qgd,kd->gqk', q_wide, ck_wide) * score_scale + lift_row[:, None, None]
            peak = jnp.maximum(lax.optimization_barrier(jnp.max(lat_scores, axis=-1)), lax.optimization_barrier(jnp.max(ctx_scores, axis=-1)))[..., None]
            lat_expo = jnp.exp(lat_scores - peak)
            ctx_expo = jnp.exp(ctx_scores - peak)
            denom = lax.optimization_barrier(jnp.sum(lat_expo, axis=-1)) + lax.optimization_barrier(jnp.sum(ctx_expo, axis=-1))
            lat_probs = lax.optimization_barrier(lat_expo.astype(jnp.bfloat16)).astype(jnp.float32)
            ctx_probs = lax.optimization_barrier(ctx_expo.astype(jnp.bfloat16)).astype(jnp.float32)
            numer = jnp.einsum('gqk,kd->gqd', lat_probs, v_wide) + jnp.einsum('gqk,kd->gqd', ctx_probs, cv_wide)
            return (numer / denom[..., None]).astype(jnp.bfloat16)
        return lax.map(per_block, blocks)
    heads_out = lax.map(per_head, (query_heads, key_heads, value_heads, ctx_key_heads, ctx_value_heads, lift_rows))
    attended = heads_out.transpose(1, 3, 0, 2, 4).reshape(SEQ, Q_HEADS * HD)
    mixed = jnp.dot(attended, out_weight, preferred_element_type=jnp.float32).astype(jnp.bfloat16)
    gate_lat = modulation[0, 2 * model_width:]
    return (latent.astype(jnp.float32) + gate_lat * mixed.astype(jnp.float32)).astype(jnp.bfloat16)
```

```python
import functools

import jax
import jax.numpy as jnp
from jax import lax
from jax.experimental import pallas as pl
from jax.experimental.pallas import tpu as pltpu
from jax.sharding import PartitionSpec as P

GRID_W = 64
EPS = 1e-06
MESH = pl.DeviceIdType.MESH
ANY = pl.BlockSpec(memory_space=pl.ANY)
VMEM = pl.BlockSpec(memory_space=pltpu.VMEM)
SMEM = pl.BlockSpec(memory_space=pltpu.SMEM)
BF16 = jnp.bfloat16
F32 = jnp.float32


def remote(src, dst, send, recv, index, axis, peer):
    return pltpu.make_async_remote_copy(
        src_ref=src, dst_ref=dst, send_sem=send.at[index], recv_sem=recv.at[index],
        device_id={axis: peer}, device_id_type=MESH,
    )


def greet(peers):
    barrier = pltpu.get_barrier_semaphore()
    for axis, peer in peers:
        pl.semaphore_signal(barrier, inc=1, device_id={axis: peer}, device_id_type=MESH)
    pl.semaphore_wait(barrier, len(peers))


def others(axis, count):
    me = lax.axis_index(axis)
    return [(axis, lax.rem(me + step, count)) for step in range(1, count)]


def gather_sems(count):
    return 13 if count == 8 else max(count - 1, 1)


class Gather:
    def __init__(self, count, own, full, send, recv):
        self.count, self.own, self.full, self.send, self.recv = count, own, full, send, recv
        self.me = lax.axis_index("tp")
        self.half = own.shape[0] // 2
        me = self.me
        if count == 8:
            self.core, self.x, self.y = me % 2, (me // 2) % 2, me // 4
            self.sib = me + 1 - 2 * self.core
            self.step = 1 - 2 * self.core
            self.xn = me + 2 - 4 * self.x
            self.yn = me + 4 - 8 * self.y
            self.dn = self.xn + 4 - 8 * self.y

    def part(self, ref, which):
        return ref if which is None else ref.at[pl.ds(which * self.half, self.half)]

    def copy(self, index):
        me, xn, yn, dn, sib = self.me, self.xn, self.yn, self.dn, self.sib
        origin, half, peer = {
            0: (me, 0, xn), 1: (me, 1, xn), 2: (me, 0, yn), 3: (me, 1, yn), 4: (me, None, sib),
            5: (xn, 1, yn), 6: (yn, 0, xn),
            7: (xn, 0, sib), 8: (xn, 1, sib), 9: (yn, 0, sib), 10: (yn, 1, sib),
            11: (dn, 0, sib), 12: (dn, 1, sib),
        }[index]
        source = self.own if index < 5 else self.full.at[origin]
        return remote(self.part(source, half), self.part(self.full.at[origin], half), self.send, self.recv, index, "tp", peer)

    def wait_recv(self, index):
        xn, yn, dn, sib, step = self.xn, self.yn, self.dn, self.sib, self.step
        origin, half = {
            0: (xn, 0), 1: (xn, 1), 2: (yn, 0), 3: (yn, 1), 4: (sib, None), 5: (dn, 1), 6: (dn, 0),
            7: (xn + step, 0), 8: (xn + step, 1), 9: (yn + step, 0), 10: (yn + step, 1),
            11: (dn + step, 0), 12: (dn + step, 1),
        }[index]
        ref = self.part(self.full.at[origin], half)
        remote(ref, ref, self.send, self.recv, index, "tp", sib).wait_recv()

    def direct(self, step):
        peer = lax.rem(self.me + step, self.count)
        return remote(self.own, self.full.at[self.me], self.send, self.recv, step - 1, "tp", peer)

    def start(self):
        if self.count == 8:
            for index in (1, 2, 0, 3, 4):
                self.copy(index).start()
        else:
            for step in range(1, self.count):
                self.direct(step).start()

    def before(self, index):
        if self.count != 8:
            @pl.when(index == 0)
            def _():
                for step in range(1, self.count):
                    origin = lax.rem(self.me - step + self.count, self.count)
                    ref = self.full.at[origin]
                    remote(ref, ref, self.send, self.recv, step - 1, "tp", origin).wait_recv()
            return

        @pl.when(index == 0)
        def _():
            self.wait_recv(4)

        @pl.when(index == 1)
        def _():
            for arrived, then in ((1, (5, 8)), (2, (6, 9)), (0, (7,)), (3, (10,))):
                self.wait_recv(arrived)
                for nxt in then:
                    self.copy(nxt).start()
            self.wait_recv(7)
            self.wait_recv(8)

        @pl.when(index == 2)
        def _():
            self.wait_recv(9)
            self.wait_recv(10)

        @pl.when(index == 3)
        def _():
            self.wait_recv(5)
            self.copy(12).start()
            self.wait_recv(6)
            self.copy(11).start()
            self.wait_recv(12)
            self.wait_recv(11)

    def chip(self, index):
        if self.count == 8:
            return ((self.y + index // 2) % 2) * 2 + (self.x + index) % 2
        return index

    def finish(self):
        if self.count == 8:
            for index in range(13):
                self.copy(index).wait_send()
        else:
            for step in range(1, self.count):
                self.direct(step).wait_send()


def front_kernel(sp, tp, head, stacked, lat, ctx, partial, gain, cos, sin, gains, *rest):
    weights, rest = rest[: 1 if stacked else 3], rest[1 if stacked else 3 :]
    qkv, gate, full, normed, wide, parts, total, mod, gsc, shf, send, recv, psend, precv, msend, mrecv, local = rest
    s, f = lax.axis_index("sp"), lax.axis_index("tp")
    rows, model = lat.shape
    width = wide.shape[2]
    slots = wide.shape[0]
    tile = 2 * rows
    mcols = partial.shape[1]
    copies = []
    if stacked:
        copies.append(pltpu.make_async_copy(weights[0], wide, local.at[0]))
    else:
        groups = slots - 2
        for n in range(groups):
            copies.append(pltpu.make_async_copy(weights[0].at[:, n * width : (n + 1) * width], wide.at[n], local.at[n]))
        copies.append(pltpu.make_async_copy(weights[1], wide.at[groups], local.at[groups]))
        copies.append(pltpu.make_async_copy(weights[2], wide.at[groups + 1], local.at[groups + 1]))
    own = pltpu.make_async_copy(lat, full.at[f], local.at[slots])
    ctx_in = [
        pltpu.make_async_copy(ctx.at[pl.ds(n * rows, rows)], full.at[tp + n], local.at[slots + 1 + n]) for n in range(2)
    ]
    greet(others("tp", tp) + others("sp", sp))
    sends = []
    for step in range(1, sp):
        sends.append(remote(partial, parts.at[s], psend, precv, step - 1, "sp", lax.rem(s + step, sp)))
    for item in sends:
        item.start()
    gather = Gather(tp, lat, full, send, recv)
    gather.start()
    for item in ctx_in + [own] + copies:
        item.start()
    parts[s] = partial[...]
    for step in range(1, sp):
        origin = lax.rem(s - step + sp, sp)
        remote(parts.at[origin], parts.at[origin], psend, precv, step - 1, "sp", origin).wait_recv()
    summed = parts[0]
    for n in range(1, sp):
        summed = summed + parts[n]
    total[...] = summed
    here = pl.ds(pl.multiple_of(f * mcols, mcols), mcols)
    mod[:, here] = summed
    outs = []
    for step in range(1, tp):
        outs.append(remote(total, mod.at[:, here], msend, mrecv, step - 1, "tp", lax.rem(f + step, tp)))
    for item in outs:
        item.start()
    for step in range(1, tp):
        origin = lax.rem(f - step + tp, tp)
        ref = mod.at[:, pl.ds(pl.multiple_of(origin * mcols, mcols), mcols)]
        remote(ref, ref, msend, mrecv, step - 1, "tp", origin).wait_recv()
    for r in range(2):
        gsc[r] = gain[...] * (1.0 + mod[r : r + 1, model : 2 * model])
        shf[r] = mod[r : r + 1, :model]
    gate[...] = mod[0:1, 2 * model :]
    for item in ctx_in + copies:
        item.wait()
    own.wait()

    lane = lax.broadcasted_iota(jnp.int32, (tile, width), 1)
    even = lane % 2 == 0
    same = (
        lax.broadcasted_iota(jnp.int32, (width, width), 0) // head
        == lax.broadcasted_iota(jnp.int32, (width, width), 1) // head
    )
    ones = jnp.where(same, 1.0, 0.0).astype(BF16)
    step_rows = 16

    def roll(v, by):
        if width % 128 == 0:
            return pltpu.roll(v, by % width, axis=1)
        return jnp.concatenate([v[:, width - by % width :], v[:, : width - by % width]], axis=1)

    def widen(v):
        if width > v.shape[1]:
            return jnp.concatenate([v] * (width // v.shape[1]), axis=1)
        return v[:, :width]

    def one_tile(number, unused):
        order = number - 1

        @pl.when(number > 0)
        def _():
            gather.before(order)

        is_ctx = jnp.where(number == 0, 1, 0)
        chip = gather.chip(jnp.maximum(order, 0))
        chip = jnp.where(number == 0, tp // 2, chip)
        first = pl.multiple_of(chip * tile, tile)

        def norm_rows(j, unused):
            slot = chip * 2 + (j * step_rows) // rows
            row = pl.multiple_of((j * step_rows) % rows, step_rows)
            v = full[slot, pl.ds(row, step_rows), :].astype(F32)
            inv = lax.rsqrt(jnp.mean(v * v, axis=-1, keepdims=True) + EPS)
            out = v * inv * gsc[is_ctx] + shf[is_ctx]
            normed[pl.ds(pl.multiple_of(j * step_rows, step_rows), step_rows), :] = out.astype(BF16)
            return unused

        lax.fori_loop(0, tile // step_rows, norm_rows, 0)

        def one_slot(n, unused):
            y = jnp.dot(normed[...], wide[n], preferred_element_type=F32)

            @pl.when(n == slots - 1)
            def _():
                qkv[n, pl.ds(first, tile), :] = y.astype(BF16)

            @pl.when(n < slots - 1)
            def _():
                sq = y * y
                hi = sq.astype(BF16)
                lo = (sq - hi.astype(F32)).astype(BF16)
                mean = jnp.dot(hi, ones, preferred_element_type=F32) + jnp.dot(lo, ones, preferred_element_type=F32)
                u = y * lax.rsqrt(mean * (1.0 / head) + EPS) * gains[n]
                other = jnp.where(even, roll(u, -1), roll(u, 1))
                turned = u * widen(cos[pl.ds(first, tile), :]) + other * widen(sin[pl.ds(first, tile), :])
                qkv[n, pl.ds(first, tile), :] = turned.astype(BF16)

            return unused

        lax.fori_loop(jnp.where(number == 0, slots - 2, 0), slots, one_slot, 0)
        return unused

    lax.fori_loop(0, tp // 2 + 1, one_tile, 0)
    for item in sends + outs:
        item.wait_send()
    gather.finish()


def attend_kernel(sp, heads, kv_heads, head, lat_rows, qkv, lift, out, kvs, top, acc, send, recv, local):
    s = lax.axis_index("sp")
    slots, rows, width = qkv.shape
    group = heads // kv_heads
    ring = sp == 4
    right, left, far = (s + 1) % sp, (s + sp - 1) % sp, (s + 2) % sp
    greet([("sp", right), ("sp", left)] if ring else others("sp", sp))
    own = qkv.at[pl.ds(slots - 2, 2)]

    def ring_copy(index):
        which, origin, peer = {
            0: (0, s, right), 1: (1, s, right), 2: (1, s, left), 3: (0, s, left), 4: (0, left, right), 5: (1, right, left),
        }[index]
        source = qkv.at[slots - 2 + which] if index < 4 else kvs.at[origin, which]
        return remote(source, kvs.at[origin, which], send, recv, index, "sp", peer)

    def ring_wait(index):
        which, origin = {0: (0, left), 1: (1, left), 2: (1, right), 3: (0, right), 4: (0, far), 5: (1, far)}[index]
        ref = kvs.at[origin, which]
        remote(ref, ref, send, recv, index, "sp", right).wait_recv()

    def direct(step):
        return remote(own, kvs.at[s], send, recv, step - 1, "sp", lax.rem(s + step, sp))

    if ring:
        for index in (0, 2, 1, 3):
            ring_copy(index).start()
    else:
        for step in range(1, sp):
            direct(step).start()
    mine = pltpu.make_async_copy(own, kvs.at[s], local)
    mine.start()
    top[...] = jnp.full(top.shape, -1e30, F32)
    acc[...] = jnp.zeros(acc.shape, F32)
    mine.wait()
    q_tile = min(256, lat_rows)
    scale = head ** -0.5

    def block(b, unused):
        if ring:
            @pl.when(b == 1)
            def _():
                ring_wait(0)
                ring_copy(4).start()
                ring_wait(2)
                ring_copy(5).start()
                ring_wait(1)

            @pl.when(b == 2)
            def _():
                ring_wait(3)

            @pl.when(b == 3)
            def _():
                ring_wait(4)
                ring_wait(5)

            origin = (s + jnp.where(b == 1, sp - 1, jnp.where(b == 2, 1, jnp.where(b == 3, 2, 0)))) % sp
        else:
            @pl.when(b == 1)
            def _():
                for step in range(1, sp):
                    source = lax.rem(s - step + sp, sp)
                    remote(kvs.at[source], kvs.at[source], send, recv, step - 1, "sp", source).wait_recv()

            origin = (s + b) % sp

        def q_rows(t, unused):
            first = pl.multiple_of(t * q_tile, q_tile)
            at = pl.ds(first, q_tile)
            for h in range(kv_heads):
                k = kvs[origin, 0, :, h * head : (h + 1) * head]
                v = kvs[origin, 1, :, h * head : (h + 1) * head]
                v_wide = jnp.concatenate([v, jnp.ones((rows, head), BF16)], axis=1)
                for g in range(group):
                    n = h * group + g
                    slot, lane = (n * head) // width, (n * head) % width
                    q = qkv[slot, at, lane : lane + head]
                    scores = lax.dot_general(q, k, (((1,), (1,)), ((), ())), preferred_element_type=F32)
                    scores = scores * scale
                    offset = jnp.where(lax.broadcasted_iota(jnp.int32, (1, rows), 1) >= lat_rows, lift[n], 0.0)
                    scores = scores + offset
                    before = top[n, at, :]
                    now = jnp.maximum(before, jnp.max(scores, axis=-1, keepdims=True))
                    expo = jnp.exp(scores - now)
                    keep = jnp.exp(before - now)
                    top[n, at, :] = now
                    acc[n, at, :] = acc[n, at, :] * keep + jnp.dot(expo.astype(BF16), v_wide, preferred_element_type=F32)
            return unused

        lax.fori_loop(0, lat_rows // q_tile, q_rows, 0)
        return unused

    lax.fori_loop(0, sp, block, 0)

    def close(t, unused):
        at = pl.ds(pl.multiple_of(t * q_tile, q_tile), q_tile)
        for pair in range(heads // 2):
            two = [acc[2 * pair + n, at, :] for n in range(2)]
            two = [v[:, :head] / v[:, head:] for v in two]
            out[at, pair * 2 * head : (pair + 1) * 2 * head] = jnp.concatenate(two, axis=1).astype(BF16)
        return unused

    lax.fori_loop(0, lat_rows // q_tile, close, 0)
    if ring:
        for index in range(6):
            ring_copy(index).wait_send()
    else:
        for step in range(1, sp):
            direct(step).wait_send()


def back_kernel(tp, att, weight, lat, gate, out, full, wide, total, mixed, landed, send, recv, asend, arecv, local):
    f = lax.axis_index("tp")
    rows, cols = att.shape
    own_rows = lat.shape[0]
    out_cols = weight.shape[1]
    load = pltpu.make_async_copy(weight, wide, local.at[0])
    load.start()
    mine = pltpu.make_async_copy(att, full.at[f], local.at[1])
    mine.start()
    greet(others("tp", tp))
    gather = Gather(tp, att, full, send, recv)
    gather.start()
    total[...] = jnp.zeros(total.shape, F32)
    mine.wait()
    load.wait()
    r_tile = min(256, rows)

    def chip_step(index, unused):
        gather.before(index)
        chip = gather.chip(index)

        def row_step(t, unused):
            at = pl.ds(pl.multiple_of(t * r_tile, r_tile), r_tile)
            value = total[at, :]
            for n in range(2):
                source = chip * 2 + n
                depth = pl.ds(pl.multiple_of(source * cols, cols), cols)
                value = value + jnp.dot(full[source, at, :], wide[depth, :], preferred_element_type=F32)
            total[at, :] = value
            return unused

        lax.fori_loop(0, rows // r_tile, row_step, 0)
        return unused

    lax.fori_loop(0, tp // 2, chip_step, 0)
    for peer in range(tp):
        mixed[peer] = total[peer * own_rows : (peer + 1) * own_rows, :].astype(BF16)
    sends = []
    for step in range(1, tp):
        peer = lax.rem(f + step, tp)
        sends.append(remote(mixed.at[peer], landed.at[f], asend, arecv, step - 1, "tp", peer))
    for item in sends:
        item.start()
    landed[f] = mixed[f]
    for step in range(1, tp):
        origin = lax.rem(f - step + tp, tp)
        remote(landed.at[origin], landed.at[origin], asend, arecv, step - 1, "tp", origin).wait_recv()
    for n in range(tp):
        at = slice(n * out_cols, (n + 1) * out_cols)
        out[:, at] = (lat[:, at].astype(F32) + gate[:, at] * landed[n].astype(F32)).astype(BF16)
    for item in sends:
        item.wait_send()
    gather.finish()


def tables(first, count, extra, head):
    freqs = head // 4
    lane = jnp.arange(2 * head, dtype=jnp.int32) % head
    pair = lane // 2
    inverse = 10000.0 ** (-(pair % freqs).astype(F32) / freqs)
    sign = jnp.where(lane % 2 == 0, -1.0, 1.0)
    by_row = pair < freqs
    grid_rows = -(-count // GRID_W) + 1
    small = jnp.concatenate([jnp.arange(grid_rows, dtype=jnp.int32) + first // GRID_W, jnp.arange(GRID_W, dtype=jnp.int32)])
    angles = small.astype(F32)[:, None] * inverse
    cos, sin = lax.optimization_barrier((jnp.cos(angles), jnp.sin(angles) * sign))

    def spread(table, fill):
        if count % GRID_W == 0:
            row = jnp.broadcast_to(table[: count // GRID_W, None, :], (count // GRID_W, GRID_W, 2 * head))
            col = jnp.broadcast_to(table[None, grid_rows:, :], row.shape)
            both = jnp.where(by_row, row, col).reshape(count, 2 * head)
        else:
            spots = first + jnp.arange(count, dtype=jnp.int32)
            both = jnp.where(by_row, table[spots // GRID_W - first // GRID_W], table[grid_rows + spots % GRID_W])
        return jnp.concatenate([both, jnp.full((extra, 2 * head), fill, F32)])

    return spread(cos, 1.0), spread(sin, 0.0)


def local(sp, tp, latent, context, condition, context_cond, mod_weight, norm_gain, query_weight, key_weight,
          value_weight, out_weight, query_gain, key_gain, context_lift):
    rows, model = latent.shape
    ctx_rows = context.shape[0]
    head = query_gain.shape[0]
    heads = query_weight.shape[1] // head
    kv_heads = key_weight.shape[1] // head
    width = key_weight.shape[1]
    slots = query_weight.shape[1] // width + 2
    block = rows * tp
    keys = block + ctx_rows
    limit = 60 * 1024 * 1024
    cond_pair = jax.nn.silu(jnp.stack([condition, context_cond])).astype(BF16)
    partial = jnp.dot(cond_pair, mod_weight, preferred_element_type=F32)
    mcols = partial.shape[1]
    cos, sin = tables(lax.axis_index("sp") * block, block, ctx_rows, head)
    gains = jnp.stack([jnp.tile(query_gain, width // head)] * (slots - 2) + [jnp.tile(key_gain, width // head)] * 2)
    gains = gains.reshape(slots, 1, width)
    stacked = width % 128 != 0
    weights = [query_weight, key_weight, value_weight]
    if stacked:
        weights = [jnp.stack([query_weight[:, n * width : (n + 1) * width] for n in range(slots - 2)] + weights[1:])]
    dma = pltpu.SemaphoreType.DMA
    count = gather_sems(tp)
    qkv, gate = pl.pallas_call(
        functools.partial(front_kernel, sp, tp, head, stacked),
        name="front",
        out_shape=(jax.ShapeDtypeStruct((slots, keys, width), BF16), jax.ShapeDtypeStruct((1, model), F32)),
        in_specs=[ANY, ANY, VMEM, VMEM, VMEM, VMEM, VMEM] + [ANY] * len(weights),
        out_specs=(VMEM, VMEM),
        scratch_shapes=[
            pltpu.VMEM((tp + 2, rows, model), BF16),
            pltpu.VMEM((2 * rows, model), BF16),
            pltpu.VMEM((slots, model, width), BF16),
            pltpu.VMEM((sp, 2, mcols), F32),
            pltpu.VMEM((2, mcols), F32),
            pltpu.VMEM((2, mcols * tp), F32),
            pltpu.VMEM((2, 1, model), F32),
            pltpu.VMEM((2, 1, model), F32),
            dma((count,)), dma((count,)), dma((sp - 1,)), dma((sp - 1,)), dma((tp - 1,)), dma((tp - 1,)),
            dma((slots + 3,)),
        ],
        compiler_params=pltpu.CompilerParams(collective_id=0, has_side_effects=True, vmem_limit_bytes=limit),
    )(latent, context, partial, norm_gain.reshape(1, model), cos, sin, gains, *weights)
    attended = pl.pallas_call(
        functools.partial(attend_kernel, sp, heads, kv_heads, head, block),
        name="attend",
        out_shape=jax.ShapeDtypeStruct((block, heads * head), BF16),
        in_specs=[VMEM, SMEM],
        out_specs=VMEM,
        scratch_shapes=[
            pltpu.VMEM((sp, 2, keys, width), BF16),
            pltpu.VMEM((heads, block, 1), F32),
            pltpu.VMEM((heads, block, 2 * head), F32),
            dma((max(sp - 1, 6),)), dma((max(sp - 1, 6),)), dma,
        ],
        compiler_params=pltpu.CompilerParams(collective_id=1, has_side_effects=True, vmem_limit_bytes=limit),
    )(qkv, context_lift)
    return pl.pallas_call(
        functools.partial(back_kernel, tp),
        name="back",
        out_shape=jax.ShapeDtypeStruct((rows, model), BF16),
        in_specs=[VMEM, ANY, VMEM, VMEM],
        out_specs=VMEM,
        scratch_shapes=[
            pltpu.VMEM((tp, block, heads * head), BF16),
            pltpu.VMEM(out_weight.shape, BF16),
            pltpu.VMEM((block, out_weight.shape[1]), F32),
            pltpu.VMEM((tp, rows, out_weight.shape[1]), BF16),
            pltpu.VMEM((tp, rows, out_weight.shape[1]), BF16),
            dma((count,)), dma((count,)), dma((tp - 1,)), dma((tp - 1,)), dma((2,)),
        ],
        compiler_params=pltpu.CompilerParams(collective_id=2, has_side_effects=True, vmem_limit_bytes=limit),
    )(attended, out_weight, latent, gate)


def solution(mesh):
    return jax.shard_map(
        functools.partial(local, mesh.shape["sp"], mesh.shape["tp"]),
        mesh=mesh,
        in_specs=(
            P(("sp", "tp"), None),
            P("sp", None),
            P("sp"),
            P("sp"),
            P("sp", "tp"),
            P(),
            P(None, "tp"),
            P(None, "tp"),
            P(None, "tp"),
            P(None, "tp"),
            P(),
            P(),
            P("tp"),
        ),
        out_specs=P(("sp", "tp"), None),
        check_vma=False,
    )
```

```python
import functools

import jax
import jax.numpy as jnp
from jax import lax
from jax.experimental import pallas as pl
from jax.experimental.pallas import tpu as pltpu
from jax.sharding import PartitionSpec as P

GRID_W = 64
EPS = 1e-06
MESH = pl.DeviceIdType.MESH
ANY = pl.BlockSpec(memory_space=pl.ANY)
VMEM = pl.BlockSpec(memory_space=pltpu.VMEM)
SMEM = pl.BlockSpec(memory_space=pltpu.SMEM)
BF16 = jnp.bfloat16
F32 = jnp.float32


def remote(src, dst, send, recv, index, axis, peer):
    return pltpu.make_async_remote_copy(
        src_ref=src, dst_ref=dst, send_sem=send.at[index], recv_sem=recv.at[index],
        device_id={axis: peer}, device_id_type=MESH,
    )


def greet(peers):
    barrier = pltpu.get_barrier_semaphore()
    for axis, peer in peers:
        pl.semaphore_signal(barrier, inc=1, device_id={axis: peer}, device_id_type=MESH)
    pl.semaphore_wait(barrier, len(peers))


def others(axis, count):
    me = lax.axis_index(axis)
    return [(axis, lax.rem(me + step, count)) for step in range(1, count)]


def gather_sems(count):
    return 13 if count == 8 else max(count - 1, 1)


class Gather:
    def __init__(self, count, own, full, send, recv):
        self.count, self.own, self.full, self.send, self.recv = count, own, full, send, recv
        self.me = lax.axis_index("tp")
        self.half = own.shape[0] // 2
        me = self.me
        if count == 8:
            self.core, self.x, self.y = me % 2, (me // 2) % 2, me // 4
            self.sib = me + 1 - 2 * self.core
            self.step = 1 - 2 * self.core
            self.xn = me + 2 - 4 * self.x
            self.yn = me + 4 - 8 * self.y
            self.dn = self.xn + 4 - 8 * self.y

    def part(self, ref, which):
        return ref if which is None else ref.at[pl.ds(which * self.half, self.half)]

    def copy(self, index):
        me, xn, yn, dn, sib = self.me, self.xn, self.yn, self.dn, self.sib
        origin, half, peer = {
            0: (me, 0, xn), 1: (me, 1, xn), 2: (me, 0, yn), 3: (me, 1, yn), 4: (me, None, sib),
            5: (xn, 1, yn), 6: (yn, 0, xn),
            7: (xn, 0, sib), 8: (xn, 1, sib), 9: (yn, 0, sib), 10: (yn, 1, sib),
            11: (dn, 0, sib), 12: (dn, 1, sib),
        }[index]
        source = self.own if index < 5 else self.full.at[origin]
        return remote(self.part(source, half), self.part(self.full.at[origin], half), self.send, self.recv, index, "tp", peer)

    def wait_recv(self, index):
        xn, yn, dn, sib, step = self.xn, self.yn, self.dn, self.sib, self.step
        origin, half = {
            0: (xn, 0), 1: (xn, 1), 2: (yn, 0), 3: (yn, 1), 4: (sib, None), 5: (dn, 1), 6: (dn, 0),
            7: (xn + step, 0), 8: (xn + step, 1), 9: (yn + step, 0), 10: (yn + step, 1),
            11: (dn + step, 0), 12: (dn + step, 1),
        }[index]
        ref = self.part(self.full.at[origin], half)
        remote(ref, ref, self.send, self.recv, index, "tp", sib).wait_recv()

    def direct(self, step):
        peer = lax.rem(self.me + step, self.count)
        return remote(self.own, self.full.at[self.me], self.send, self.recv, step - 1, "tp", peer)

    def start(self):
        if self.count == 8:
            for index in (1, 2, 4):
                self.copy(index).start()
        else:
            for step in range(1, self.count):
                self.direct(step).start()

    def second(self):
        if self.count == 8:
            for index in (0, 3):
                self.copy(index).start()

    def relay(self):
        if self.count == 8:
            for arrived, then in ((1, (5, 8)), (2, (6, 9))):
                self.wait_recv(arrived)
                for nxt in then:
                    self.copy(nxt).start()

    def before(self, index):
        if self.count != 8:
            @pl.when(index == 0)
            def _():
                for step in range(1, self.count):
                    origin = lax.rem(self.me - step + self.count, self.count)
                    ref = self.full.at[origin]
                    remote(ref, ref, self.send, self.recv, step - 1, "tp", origin).wait_recv()
            return

        @pl.when(index == 0)
        def _():
            self.wait_recv(4)

        @pl.when(index == 1)
        def _():
            for arrived, nxt in ((0, 7), (3, 10)):
                self.wait_recv(arrived)
                self.copy(nxt).start()
            self.wait_recv(7)
            self.wait_recv(8)

        @pl.when(index == 2)
        def _():
            self.wait_recv(9)
            self.wait_recv(10)

        @pl.when(index == 3)
        def _():
            self.wait_recv(5)
            self.copy(12).start()
            self.wait_recv(6)
            self.copy(11).start()
            self.wait_recv(12)
            self.wait_recv(11)

    def chip(self, index):
        if self.count == 8:
            return ((self.y + index // 2) % 2) * 2 + (self.x + index) % 2
        return index

    def finish(self):
        if self.count == 8:
            for index in range(13):
                self.copy(index).wait_send()
        else:
            for step in range(1, self.count):
                self.direct(step).wait_send()


def front_kernel(sp, tp, heads, kv_heads, head, stacked, lat, ctx, cond, mod_weight, gain, cos, sin, q_gain, k_gain, lift, *rest):
    weights, rest = rest[: 1 if stacked else 3], rest[1 if stacked else 3 :]
    (attended, gate, full, normed, wide, mod_wide, parts, partial, total, mod, gsc, shf, gains, q_all, kvs, top, acc,
     send, recv, psend, precv, msend, mrecv, zsend, zrecv, local) = rest
    s, f = lax.axis_index("sp"), lax.axis_index("tp")
    rows, model = lat.shape
    width = wide.shape[2]
    slots = wide.shape[0]
    groups = slots - 2
    tile = 2 * rows
    lat_rows = rows * tp
    keys = kvs.shape[2]
    mcols = partial.shape[1]
    tiles = tp // 2 + 1
    mod_in = pltpu.make_async_copy(mod_weight, mod_wide, local.at[slots + 3])
    mod_in.start()
    copies = []
    if stacked:
        copies.append(pltpu.make_async_copy(weights[0], wide, local.at[0]))
    else:
        for n in range(groups):
            copies.append(pltpu.make_async_copy(weights[0].at[:, n * width : (n + 1) * width], wide.at[n], local.at[n]))
        copies.append(pltpu.make_async_copy(weights[1], wide.at[groups], local.at[groups]))
        copies.append(pltpu.make_async_copy(weights[2], wide.at[groups + 1], local.at[groups + 1]))
    own = pltpu.make_async_copy(lat, full.at[f], local.at[slots])
    ctx_in = [
        pltpu.make_async_copy(ctx.at[pl.ds(n * rows, rows)], full.at[tp + n], local.at[slots + 1 + n]) for n in range(2)
    ]
    greet(others("tp", tp) + others("sp", sp))
    gather = Gather(tp, lat, full, send, recv)
    gather.start()
    for item in ctx_in + [own] + copies[::-1]:
        item.start()
    mod_in.wait()
    first_sum = jnp.dot(cond[...], mod_wide[...], preferred_element_type=F32)
    partial[...] = first_sum
    parts[s] = first_sum
    sends = []
    for step in range(1, sp):
        sends.append(remote(partial, parts.at[s], psend, precv, step - 1, "sp", lax.rem(s + step, sp)))
    for item in sends:
        item.start()
    for n in range(slots):
        row = (q_gain if n < groups else k_gain)[...]
        gains[n] = jnp.concatenate([row] * (width // head), axis=1) if width > head else row
    for step in range(1, sp):
        origin = lax.rem(s - step + sp, sp)
        remote(parts.at[origin], parts.at[origin], psend, precv, step - 1, "sp", origin).wait_recv()
    summed = parts[0]
    for n in range(1, sp):
        summed = summed + parts[n]
    total[...] = summed
    here = pl.ds(pl.multiple_of(f * mcols, mcols), mcols)
    mod[:, here] = summed
    outs = []
    for step in range(1, tp):
        outs.append(remote(total, mod.at[:, here], msend, mrecv, step - 1, "tp", lax.rem(f + step, tp)))
    for item in outs:
        item.start()
    gather.second()
    top[...] = jnp.full(top.shape, -1e30, F32)
    acc[...] = jnp.zeros(acc.shape, F32)
    for step in range(1, tp):
        origin = lax.rem(f - step + tp, tp)
        ref = mod.at[:, pl.ds(pl.multiple_of(origin * mcols, mcols), mcols)]
        remote(ref, ref, msend, mrecv, step - 1, "tp", origin).wait_recv()
    for r in range(2):
        gsc[r] = gain[...] * (1.0 + mod[r : r + 1, model : 2 * model])
        shf[r] = mod[r : r + 1, :model]
    gate[...] = mod[0:1, 2 * model :]
    gather.relay()
    for item in ctx_in + copies:
        item.wait()
    own.wait()

    ring = sp == 4
    right, left, far = (s + 1) % sp, (s + sp - 1) % sp, (s + 2) % sp

    def tile_first(number):
        if isinstance(number, int):
            return lat_rows if number == 0 else pl.multiple_of(gather.chip(number - 1) * tile, tile)
        chip = jnp.where(number == 0, tp // 2, gather.chip(jnp.maximum(number - 1, 0)))
        return pl.multiple_of(chip * tile, tile)

    def ring_copy(number, index):
        which, origin, peer = {
            0: (0, s, right), 1: (1, s, right), 2: (1, s, left), 3: (0, s, left), 4: (0, left, right), 5: (1, right, left),
        }[index]
        ref = kvs.at[origin, which, pl.ds(tile_first(number), tile)]
        return remote(ref, ref, zsend, zrecv, number * 6 + index, "sp", peer)

    def ring_wait(number, index):
        which, origin = {0: (0, left), 1: (1, left), 2: (1, right), 3: (0, right), 4: (0, far), 5: (1, far)}[index]
        ref = kvs.at[origin, which, pl.ds(tile_first(number), tile)]
        remote(ref, ref, zsend, zrecv, number * 6 + index, "sp", right).wait_recv()

    def forward(number):
        ring_wait(number, 0)
        ring_copy(number, 4).start()
        ring_wait(number, 2)
        ring_copy(number, 5).start()

    def direct(step):
        return remote(kvs.at[s], kvs.at[s], zsend, zrecv, step - 1, "sp", lax.rem(s + step, sp))

    even = lax.broadcasted_iota(jnp.int32, (tile, width), 1) % 2 == 0
    same = (
        lax.broadcasted_iota(jnp.int32, (width, width), 0) // head
        == lax.broadcasted_iota(jnp.int32, (width, width), 1) // head
    )
    ones = jnp.where(same, 1.0, 0.0).astype(BF16)
    by_row = (lax.broadcasted_iota(jnp.int32, (1, 2 * head), 1) % head) // 2 < head // 4
    grid_rows = cos.shape[0] - GRID_W
    part = min(tile, GRID_W)
    step_rows = 16

    def roll(v, by):
        if width % 128 == 0:
            return pltpu.roll(v, by % width, axis=1)
        return jnp.concatenate([v[:, width - by % width :], v[:, : width - by % width]], axis=1)

    def table(ref, first, is_ctx, fill):
        pieces = []
        for k in range(tile // part):
            at = jnp.where(is_ctx == 1, 0, first + k * part)
            row = ref[pl.ds(at // GRID_W, 1), :]
            col = ref[pl.ds(pl.multiple_of(grid_rows + at % GRID_W, 8), part), :]
            pieces.append(jnp.where(by_row, row, col))
        v = jnp.concatenate(pieces, axis=0) if len(pieces) > 1 else pieces[0]
        v = jnp.where(is_ctx == 1, fill, v)
        if width > v.shape[1]:
            return jnp.concatenate([v] * (width // v.shape[1]), axis=1)
        return v[:, :width]

    def one_tile(number, unused):
        @pl.when(number > 0)
        def _():
            gather.before(number - 1)

        is_ctx = jnp.where(number == 0, 1, 0)
        first = tile_first(number)
        base = first // rows

        def norm_rows(j, unused):
            slot = base + (j * step_rows) // rows
            row = pl.multiple_of((j * step_rows) % rows, step_rows)
            v = full[slot, pl.ds(row, step_rows), :].astype(F32)
            inv = lax.rsqrt(jnp.mean(v * v, axis=-1, keepdims=True) + EPS)
            out = v * inv * gsc[is_ctx] + shf[is_ctx]
            normed[pl.ds(pl.multiple_of(j * step_rows, step_rows), step_rows), :] = out.astype(BF16)
            return unused

        lax.fori_loop(0, tile // step_rows, norm_rows, 0)

        def turned(y, n):
            sq = y * y
            hi = sq.astype(BF16)
            lo = (sq - hi.astype(F32)).astype(BF16)
            mean = jnp.dot(hi, ones, preferred_element_type=F32) + jnp.dot(lo, ones, preferred_element_type=F32)
            u = y * lax.rsqrt(mean * (1.0 / head) + EPS) * gains[n]
            other = jnp.where(even, roll(u, -1), roll(u, 1))
            return (u * table(cos, first, is_ctx, 1.0) + other * table(sin, first, is_ctx, 0.0)).astype(BF16)

        def one_slot(m, unused):
            n = (m + groups) % slots
            y = jnp.dot(normed[...], wide[n], preferred_element_type=F32)

            @pl.when(m == 1)
            def _():
                kvs[s, 1, pl.ds(first, tile), :] = y.astype(BF16)
                if ring:
                    for index in (0, 2, 1, 3):
                        ring_copy(number, index).start()

            @pl.when(m == 0)
            def _():
                kvs[s, 0, pl.ds(first, tile), :] = turned(y, n)

            @pl.when(m > 1)
            def _():
                q_all[n, pl.ds(first, tile), :] = turned(y, n)

            return unused

        lax.fori_loop(0, jnp.where(number == 0, 2, slots), one_slot, 0)
        return unused

    lax.fori_loop(0, tiles, one_tile, 0)

    if not ring:
        for step in range(1, sp):
            direct(step).start()
    group = heads // kv_heads
    q_tile = min(256, lat_rows)
    q_tiles = lat_rows // q_tile
    scale = head ** -0.5

    def block(b, unused):
        if ring:
            @pl.when(b == 0)
            def _():
                for number in range(tiles - 2):
                    forward(number)

            @pl.when(b == 1)
            def _():
                forward(tiles - 1)
                for number in range(tiles):
                    ring_wait(number, 1)

            @pl.when(b == 2)
            def _():
                for number in range(tiles):
                    ring_wait(number, 3)

            @pl.when(b == 3)
            def _():
                for number in range(tiles):
                    ring_wait(number, 4)
                    ring_wait(number, 5)

            origin = (s + jnp.where(b == 1, sp - 1, jnp.where(b == 2, 1, jnp.where(b == 3, 2, 0)))) % sp
        else:
            @pl.when(b == 1)
            def _():
                for step in range(1, sp):
                    source = lax.rem(s - step + sp, sp)
                    remote(kvs.at[source], kvs.at[source], zsend, zrecv, step - 1, "sp", source).wait_recv()

            origin = (s + b) % sp

        def q_rows(t, unused):
            if ring:
                @pl.when((b == 0) & (t == q_tiles - 1))
                def _():
                    forward(tiles - 2)

            at = pl.ds(pl.multiple_of(t * q_tile, q_tile), q_tile)
            for h in range(kv_heads):
                k = kvs[origin, 0, :, h * head : (h + 1) * head]
                v = kvs[origin, 1, :, h * head : (h + 1) * head]
                v_wide = jnp.concatenate([v, jnp.ones((keys, head), BF16)], axis=1)
                for g in range(group):
                    n = h * group + g
                    slot, lane = (n * head) // width, (n * head) % width
                    q = q_all[slot, at, lane : lane + head]
                    scores = lax.dot_general(q, k, (((1,), (1,)), ((), ())), preferred_element_type=F32)
                    scores = scores * scale
                    offset = jnp.where(lax.broadcasted_iota(jnp.int32, (1, keys), 1) >= lat_rows, lift[n], 0.0)
                    scores = scores + offset
                    before = top[n, at, :]
                    now = jnp.maximum(before, jnp.max(scores, axis=-1, keepdims=True))
                    expo = jnp.exp(scores - now)
                    keep = jnp.exp(before - now)
                    top[n, at, :] = now
                    acc[n, at, :] = acc[n, at, :] * keep + jnp.dot(expo.astype(BF16), v_wide, preferred_element_type=F32)
            return unused

        lax.fori_loop(0, q_tiles, q_rows, 0)
        return unused

    lax.fori_loop(0, sp, block, 0)

    def close(t, unused):
        at = pl.ds(pl.multiple_of(t * q_tile, q_tile), q_tile)
        for pair in range(heads // 2):
            two = [acc[2 * pair + n, at, :] for n in range(2)]
            two = [v[:, :head] / v[:, head:] for v in two]
            attended[at, pair * 2 * head : (pair + 1) * 2 * head] = jnp.concatenate(two, axis=1).astype(BF16)
        return unused

    lax.fori_loop(0, q_tiles, close, 0)
    if ring:
        for number in range(tiles):
            for index in range(6):
                ring_copy(number, index).wait_send()
    else:
        for step in range(1, sp):
            direct(step).wait_send()
    for item in sends + outs:
        item.wait_send()
    gather.finish()


def back_kernel(tp, att, weight, out, full, wide, total, mixed, landed, send, recv, asend, arecv, local):
    f = lax.axis_index("tp")
    rows, cols = att.shape
    own_rows = out.shape[0]
    out_cols = weight.shape[1]
    load = pltpu.make_async_copy(weight, wide, local.at[0])
    load.start()
    mine = pltpu.make_async_copy(att, full.at[f], local.at[1])
    mine.start()
    greet(others("tp", tp))
    gather = Gather(tp, att, full, send, recv)
    gather.start()
    gather.second()
    total[...] = jnp.zeros(total.shape, F32)
    gather.relay()
    mine.wait()
    load.wait()
    r_tile = min(256, rows)

    def chip_step(index, unused):
        gather.before(index)
        chip = gather.chip(index)

        def row_step(t, unused):
            at = pl.ds(pl.multiple_of(t * r_tile, r_tile), r_tile)
            value = total[at, :]
            for n in range(2):
                source = chip * 2 + n
                depth = pl.ds(pl.multiple_of(source * cols, cols), cols)
                value = value + jnp.dot(full[source, at, :], wide[depth, :], preferred_element_type=F32)
            total[at, :] = value
            return unused

        lax.fori_loop(0, rows // r_tile, row_step, 0)
        return unused

    lax.fori_loop(0, tp // 2, chip_step, 0)
    for peer in range(tp):
        mixed[peer] = total[peer * own_rows : (peer + 1) * own_rows, :].astype(BF16)
    sends = []
    for step in range(1, tp):
        peer = lax.rem(f + step, tp)
        sends.append(remote(mixed.at[peer], landed.at[f], asend, arecv, step - 1, "tp", peer))
    for item in sends:
        item.start()
    landed[f] = mixed[f]
    for step in range(1, tp):
        origin = lax.rem(f - step + tp, tp)
        remote(landed.at[origin], landed.at[origin], asend, arecv, step - 1, "tp", origin).wait_recv()
    for n in range(tp):
        out[:, n * out_cols : (n + 1) * out_cols] = landed[n]
    for item in sends:
        item.wait_send()
    gather.finish()


def tables(first, count, head):
    freqs = head // 4
    lane = jnp.arange(2 * head, dtype=jnp.int32) % head
    inverse = 10000.0 ** (-(lane // 2 % freqs).astype(F32) / freqs)
    sign = jnp.where(lane % 2 == 0, -1.0, 1.0)
    grid_rows = -(-(count // GRID_W) // 8) * 8
    index = jnp.arange(grid_rows + GRID_W, dtype=jnp.int32)
    spot = jnp.where(index < grid_rows, index + first // GRID_W, index - grid_rows)
    angles = spot.astype(F32)[:, None] * inverse
    return jnp.cos(angles), jnp.sin(angles) * sign


def local(sp, tp, latent, context, condition, context_cond, mod_weight, norm_gain, query_weight, key_weight,
          value_weight, out_weight, query_gain, key_gain, context_lift):
    rows, model = latent.shape
    ctx_rows = context.shape[0]
    head = query_gain.shape[0]
    heads = query_weight.shape[1] // head
    kv_heads = key_weight.shape[1] // head
    width = key_weight.shape[1]
    slots = query_weight.shape[1] // width + 2
    block = rows * tp
    keys = block + ctx_rows
    limit = 60 * 1024 * 1024
    cond_pair = jax.nn.silu(jnp.stack([condition, context_cond])).astype(BF16)
    mcols = mod_weight.shape[1]
    cos, sin = tables(lax.axis_index("sp") * block, block, head)
    stacked = width % 128 != 0
    weights = [query_weight, key_weight, value_weight]
    if stacked:
        weights = [jnp.stack([query_weight[:, n * width : (n + 1) * width] for n in range(slots - 2)] + weights[1:])]
    dma = pltpu.SemaphoreType.DMA
    count = gather_sems(tp)
    pieces = (tp // 2 + 1) * 6 if sp == 4 else sp - 1
    attended, gate = pl.pallas_call(
        functools.partial(front_kernel, sp, tp, heads, kv_heads, head, stacked),
        name="front",
        out_shape=(jax.ShapeDtypeStruct((block, heads * head), BF16), jax.ShapeDtypeStruct((1, model), F32)),
        in_specs=[ANY, ANY, VMEM, ANY, VMEM, VMEM, VMEM, VMEM, VMEM, SMEM] + [ANY] * len(weights),
        out_specs=(VMEM, VMEM),
        scratch_shapes=[
            pltpu.VMEM((tp + 2, rows, model), BF16),
            pltpu.VMEM((2 * rows, model), BF16),
            pltpu.VMEM((slots, model, width), BF16),
            pltpu.VMEM(mod_weight.shape, BF16),
            pltpu.VMEM((sp, 2, mcols), F32),
            pltpu.VMEM((2, mcols), F32),
            pltpu.VMEM((2, mcols), F32),
            pltpu.VMEM((2, mcols * tp), F32),
            pltpu.VMEM((2, 1, model), F32),
            pltpu.VMEM((2, 1, model), F32),
            pltpu.VMEM((slots, 1, width), F32),
            pltpu.VMEM((slots - 2, block, width), BF16),
            pltpu.VMEM((sp, 2, keys, width), BF16),
            pltpu.VMEM((heads, block, 1), F32),
            pltpu.VMEM((heads, block, 2 * head), F32),
            dma((count,)), dma((count,)), dma((sp - 1,)), dma((sp - 1,)), dma((tp - 1,)), dma((tp - 1,)),
            dma((pieces,)), dma((pieces,)),
            dma((slots + 4,)),
        ],
        compiler_params=pltpu.CompilerParams(collective_id=0, has_side_effects=True, vmem_limit_bytes=limit),
    )(latent, context, cond_pair, mod_weight, norm_gain.reshape(1, model), cos, sin, query_gain.reshape(1, head),
      key_gain.reshape(1, head), context_lift, *weights)
    mixed = pl.pallas_call(
        functools.partial(back_kernel, tp),
        name="back",
        out_shape=jax.ShapeDtypeStruct((rows, model), BF16),
        in_specs=[VMEM, ANY],
        out_specs=VMEM,
        scratch_shapes=[
            pltpu.VMEM((tp, block, heads * head), BF16),
            pltpu.VMEM(out_weight.shape, BF16),
            pltpu.VMEM((block, out_weight.shape[1]), F32),
            pltpu.VMEM((tp, rows, out_weight.shape[1]), BF16),
            pltpu.VMEM((tp, rows, out_weight.shape[1]), BF16),
            dma((count,)), dma((count,)), dma((tp - 1,)), dma((tp - 1,)), dma((2,)),
        ],
        compiler_params=pltpu.CompilerParams(collective_id=2, has_side_effects=True, vmem_limit_bytes=limit),
    )(attended, out_weight)
    return (latent.astype(F32) + gate * mixed.astype(F32)).astype(BF16)


def solution(mesh):
    return jax.shard_map(
        functools.partial(local, mesh.shape["sp"], mesh.shape["tp"]),
        mesh=mesh,
        in_specs=(
            P(("sp", "tp"), None),
            P("sp", None),
            P("sp"),
            P("sp"),
            P("sp", "tp"),
            P(),
            P(None, "tp"),
            P(None, "tp"),
            P(None, "tp"),
            P(None, "tp"),
            P(),
            P(),
            P("tp"),
        ),
        out_specs=P(("sp", "tp"), None),
        check_vma=False,
    )
```

```python
import functools

import jax
import jax.numpy as jnp
from jax import lax
from jax.experimental import pallas as pl
from jax.experimental.pallas import tpu as pltpu
from jax.sharding import PartitionSpec as P

GRID_W = 64
EPS = 1e-06
MESH = pl.DeviceIdType.MESH
ANY = pl.BlockSpec(memory_space=pl.ANY)
VMEM = pl.BlockSpec(memory_space=pltpu.VMEM)
SMEM = pl.BlockSpec(memory_space=pltpu.SMEM)
BF16 = jnp.bfloat16
F32 = jnp.float32


def remote(src, dst, send, recv, index, axis, peer):
    return pltpu.make_async_remote_copy(
        src_ref=src, dst_ref=dst, send_sem=send.at[index], recv_sem=recv.at[index],
        device_id={axis: peer}, device_id_type=MESH,
    )


def greet(peers):
    barrier = pltpu.get_barrier_semaphore()
    for axis, peer in peers:
        pl.semaphore_signal(barrier, inc=1, device_id={axis: peer}, device_id_type=MESH)
    pl.semaphore_wait(barrier, len(peers))


def others(axis, count):
    me = lax.axis_index(axis)
    return [(axis, lax.rem(me + step, count)) for step in range(1, count)]


def gather_sems(count):
    return 13 if count == 8 else max(count - 1, 1)


class Gather:
    def __init__(self, count, own, full, send, recv):
        self.count, self.own, self.full, self.send, self.recv = count, own, full, send, recv
        self.me = lax.axis_index("tp")
        self.half = own.shape[0] // 2
        me = self.me
        if count == 8:
            self.core, self.x, self.y = me % 2, (me // 2) % 2, me // 4
            self.sib = me + 1 - 2 * self.core
            self.step = 1 - 2 * self.core
            self.xn = me + 2 - 4 * self.x
            self.yn = me + 4 - 8 * self.y
            self.dn = self.xn + 4 - 8 * self.y

    def part(self, ref, which):
        return ref if which is None else ref.at[pl.ds(which * self.half, self.half)]

    def copy(self, index):
        me, xn, yn, dn, sib = self.me, self.xn, self.yn, self.dn, self.sib
        origin, half, peer = {
            0: (me, 0, xn), 1: (me, 1, xn), 2: (me, 0, yn), 3: (me, 1, yn), 4: (me, None, sib),
            5: (xn, 1, yn), 6: (yn, 0, xn),
            7: (xn, 0, sib), 8: (xn, 1, sib), 9: (yn, 0, sib), 10: (yn, 1, sib),
            11: (dn, 0, sib), 12: (dn, 1, sib),
        }[index]
        source = self.own if index < 5 else self.full.at[origin]
        return remote(self.part(source, half), self.part(self.full.at[origin], half), self.send, self.recv, index, "tp", peer)

    def wait_recv(self, index):
        xn, yn, dn, sib, step = self.xn, self.yn, self.dn, self.sib, self.step
        origin, half = {
            0: (xn, 0), 1: (xn, 1), 2: (yn, 0), 3: (yn, 1), 4: (sib, None), 5: (dn, 1), 6: (dn, 0),
            7: (xn + step, 0), 8: (xn + step, 1), 9: (yn + step, 0), 10: (yn + step, 1),
            11: (dn + step, 0), 12: (dn + step, 1),
        }[index]
        ref = self.part(self.full.at[origin], half)
        remote(ref, ref, self.send, self.recv, index, "tp", sib).wait_recv()

    def direct(self, step):
        peer = lax.rem(self.me + step, self.count)
        return remote(self.own, self.full.at[self.me], self.send, self.recv, step - 1, "tp", peer)

    def start(self):
        if self.count == 8:
            for index in (1, 2, 4):
                self.copy(index).start()
        else:
            for step in range(1, self.count):
                self.direct(step).start()

    def second(self):
        if self.count == 8:
            for index in (0, 3):
                self.copy(index).start()

    def relay(self):
        if self.count == 8:
            for arrived, then in ((1, (5, 8)), (2, (6, 9))):
                self.wait_recv(arrived)
                for nxt in then:
                    self.copy(nxt).start()

    def before(self, index):
        if self.count != 8:
            @pl.when(index == 0)
            def _():
                for step in range(1, self.count):
                    origin = lax.rem(self.me - step + self.count, self.count)
                    ref = self.full.at[origin]
                    remote(ref, ref, self.send, self.recv, step - 1, "tp", origin).wait_recv()
            return

        @pl.when(index == 0)
        def _():
            self.wait_recv(4)

        @pl.when(index == 1)
        def _():
            for arrived, nxt in ((0, 7), (3, 10)):
                self.wait_recv(arrived)
                self.copy(nxt).start()
            self.wait_recv(7)
            self.wait_recv(8)

        @pl.when(index == 2)
        def _():
            self.wait_recv(9)
            self.wait_recv(10)

        @pl.when(index == 3)
        def _():
            self.wait_recv(5)
            self.copy(12).start()
            self.wait_recv(6)
            self.copy(11).start()
            self.wait_recv(12)
            self.wait_recv(11)

    def chip(self, index):
        if self.count == 8:
            return ((self.y + index // 2) % 2) * 2 + (self.x + index) % 2
        return index

    def finish(self):
        if self.count == 8:
            for index in range(13):
                self.copy(index).wait_send()
        else:
            for step in range(1, self.count):
                self.direct(step).wait_send()


def front_kernel(sp, tp, heads, kv_heads, head, stacked, lat, ctx, cond, mod_weight, gain, cos, sin, q_gain, k_gain, lift, *rest):
    weights, rest = rest[: 1 if stacked else 3], rest[1 if stacked else 3 :]
    (attended, gate, full, normed, wide, mod_wide, parts, partial, total, mod, gsc, shf, gains, q_all, kvs, top, acc,
     send, recv, psend, precv, msend, mrecv, zsend, zrecv, local) = rest
    s, f = lax.axis_index("sp"), lax.axis_index("tp")
    rows, model = lat.shape
    width = wide.shape[2]
    slots = wide.shape[0]
    groups = slots - 2
    tile = 2 * rows
    lat_rows = rows * tp
    keys = kvs.shape[2]
    mcols = partial.shape[1]
    tiles = tp // 2 + 1
    scale = head ** -0.5
    mod_in = pltpu.make_async_copy(mod_weight, mod_wide, local.at[slots + 3])
    mod_in.start()
    copies = []
    if stacked:
        copies.append(pltpu.make_async_copy(weights[0], wide, local.at[0]))
    else:
        for n in range(groups):
            copies.append(pltpu.make_async_copy(weights[0].at[:, n * width : (n + 1) * width], wide.at[n], local.at[n]))
        copies.append(pltpu.make_async_copy(weights[1], wide.at[groups], local.at[groups]))
        copies.append(pltpu.make_async_copy(weights[2], wide.at[groups + 1], local.at[groups + 1]))
    own = pltpu.make_async_copy(lat, full.at[f], local.at[slots])
    ctx_in = [
        pltpu.make_async_copy(ctx.at[pl.ds(n * rows, rows)], full.at[tp + n], local.at[slots + 1 + n]) for n in range(2)
    ]
    greet(others("tp", tp) + others("sp", sp))
    gather = Gather(tp, lat, full, send, recv)
    gather.start()
    for item in ctx_in + [own] + copies[::-1]:
        item.start()
    mod_in.wait()
    first_sum = jnp.dot(cond[...], mod_wide[...], preferred_element_type=F32)
    partial[...] = first_sum
    parts[s] = first_sum
    sends = []
    for step in range(1, sp):
        sends.append(remote(partial, parts.at[s], psend, precv, step - 1, "sp", lax.rem(s + step, sp)))
    for item in sends:
        item.start()
    for n in range(slots):
        row = q_gain[...] * scale if n < groups else k_gain[...]
        gains[n] = jnp.concatenate([row] * (width // head), axis=1) if width > head else row
    for step in range(1, sp):
        origin = lax.rem(s - step + sp, sp)
        remote(parts.at[origin], parts.at[origin], psend, precv, step - 1, "sp", origin).wait_recv()
    summed = parts[0]
    for n in range(1, sp):
        summed = summed + parts[n]
    total[...] = summed
    here = pl.ds(pl.multiple_of(f * mcols, mcols), mcols)
    mod[:, here] = summed
    outs = []
    for step in range(1, tp):
        outs.append(remote(total, mod.at[:, here], msend, mrecv, step - 1, "tp", lax.rem(f + step, tp)))
    for item in outs:
        item.start()
    gather.second()
    top[...] = jnp.full(top.shape, -1e30, F32)
    acc[...] = jnp.zeros(acc.shape, F32)
    for step in range(1, tp):
        origin = lax.rem(f - step + tp, tp)
        ref = mod.at[:, pl.ds(pl.multiple_of(origin * mcols, mcols), mcols)]
        remote(ref, ref, msend, mrecv, step - 1, "tp", origin).wait_recv()
    for r in range(2):
        gsc[r] = gain[...] * (1.0 + mod[r : r + 1, model : 2 * model])
        shf[r] = mod[r : r + 1, :model]
    gate[...] = mod[0:1, 2 * model :]
    gather.relay()
    for item in ctx_in + copies:
        item.wait()
    own.wait()

    ring = sp == 4
    right, left, far = (s + 1) % sp, (s + sp - 1) % sp, (s + 2) % sp

    def tile_first(number):
        if isinstance(number, int):
            return lat_rows if number == 0 else pl.multiple_of(gather.chip(number - 1) * tile, tile)
        chip = jnp.where(number == 0, tp // 2, gather.chip(jnp.maximum(number - 1, 0)))
        return pl.multiple_of(chip * tile, tile)

    def ring_copy(number, index):
        which, origin, peer = {
            0: (0, s, right), 1: (1, s, right), 2: (1, s, left), 3: (0, s, left), 4: (0, left, right), 5: (1, right, left),
        }[index]
        ref = kvs.at[origin, which, pl.ds(tile_first(number), tile)]
        return remote(ref, ref, zsend, zrecv, number * 6 + index, "sp", peer)

    def ring_wait(number, index):
        which, origin = {0: (0, left), 1: (1, left), 2: (1, right), 3: (0, right), 4: (0, far), 5: (1, far)}[index]
        ref = kvs.at[origin, which, pl.ds(tile_first(number), tile)]
        remote(ref, ref, zsend, zrecv, number * 6 + index, "sp", right).wait_recv()

    def forward(number):
        ring_wait(number, 0)
        ring_copy(number, 4).start()
        ring_wait(number, 2)
        ring_copy(number, 5).start()

    def direct(step):
        return remote(kvs.at[s], kvs.at[s], zsend, zrecv, step - 1, "sp", lax.rem(s + step, sp))

    even = lax.broadcasted_iota(jnp.int32, (tile, width), 1) % 2 == 0
    same = (
        lax.broadcasted_iota(jnp.int32, (width, width), 0) // head
        == lax.broadcasted_iota(jnp.int32, (width, width), 1) // head
    )
    ones = jnp.where(same, 1.0, 0.0).astype(BF16)
    by_row = (lax.broadcasted_iota(jnp.int32, (1, 2 * head), 1) % head) // 2 < head // 4
    grid_rows = cos.shape[0] - GRID_W
    part = min(tile, GRID_W)
    step_rows = 16

    def roll(v, by):
        if width % 128 == 0:
            return pltpu.roll(v, by % width, axis=1)
        return jnp.concatenate([v[:, width - by % width :], v[:, : width - by % width]], axis=1)

    def table(ref, first, is_ctx, fill):
        pieces = []
        for k in range(tile // part):
            at = jnp.where(is_ctx == 1, 0, first + k * part)
            row = ref[pl.ds(at // GRID_W, 1), :]
            col = ref[pl.ds(pl.multiple_of(grid_rows + at % GRID_W, 8), part), :]
            pieces.append(jnp.where(by_row, row, col))
        v = jnp.concatenate(pieces, axis=0) if len(pieces) > 1 else pieces[0]
        v = jnp.where(is_ctx == 1, fill, v)
        if width > v.shape[1]:
            return jnp.concatenate([v] * (width // v.shape[1]), axis=1)
        return v[:, :width]

    def one_tile(number, unused):
        @pl.when(number > 0)
        def _():
            gather.before(number - 1)

        is_ctx = jnp.where(number == 0, 1, 0)
        first = tile_first(number)
        base = first // rows

        def norm_rows(j, unused):
            slot = base + (j * step_rows) // rows
            row = pl.multiple_of((j * step_rows) % rows, step_rows)
            v = full[slot, pl.ds(row, step_rows), :].astype(F32)
            inv = lax.rsqrt(jnp.mean(v * v, axis=-1, keepdims=True) + EPS)
            out = v * inv * gsc[is_ctx] + shf[is_ctx]
            normed[pl.ds(pl.multiple_of(j * step_rows, step_rows), step_rows), :] = out.astype(BF16)
            return unused

        lax.fori_loop(0, tile // step_rows, norm_rows, 0)

        def turned(y, n):
            sq = y * y
            hi = sq.astype(BF16)
            lo = (sq - hi.astype(F32)).astype(BF16)
            mean = jnp.dot(hi, ones, preferred_element_type=F32) + jnp.dot(lo, ones, preferred_element_type=F32)
            u = y * lax.rsqrt(mean * (1.0 / head) + EPS) * gains[n]
            other = jnp.where(even, roll(u, -1), roll(u, 1))
            return (u * table(cos, first, is_ctx, 1.0) + other * table(sin, first, is_ctx, 0.0)).astype(BF16)

        def one_slot(m, unused):
            n = (m + groups) % slots
            y = jnp.dot(normed[...], wide[n], preferred_element_type=F32)

            @pl.when(m == 1)
            def _():
                kvs[s, 1, pl.ds(first, tile), :] = y.astype(BF16)
                if ring:
                    for index in (0, 2, 1, 3):
                        ring_copy(number, index).start()

            @pl.when(m == 0)
            def _():
                kvs[s, 0, pl.ds(first, tile), :] = turned(y, n)

            @pl.when(m > 1)
            def _():
                q_all[n, pl.ds(first, tile), :] = turned(y, n)

            return unused

        lax.fori_loop(0, jnp.where(number == 0, 2, slots), one_slot, 0)
        return unused

    lax.fori_loop(0, tiles, one_tile, 0)

    if not ring:
        for step in range(1, sp):
            direct(step).start()
    group = heads // kv_heads
    q_tile = min(256, lat_rows)
    q_tiles = lat_rows // q_tile

    def block(b, unused):
        if ring:
            @pl.when(b == 0)
            def _():
                for number in range(tiles - 2):
                    forward(number)

            @pl.when(b == 1)
            def _():
                forward(tiles - 1)
                for number in range(tiles):
                    ring_wait(number, 1)

            @pl.when(b == 2)
            def _():
                for number in range(tiles):
                    ring_wait(number, 3)

            @pl.when(b == 3)
            def _():
                for number in range(tiles):
                    ring_wait(number, 4)
                    ring_wait(number, 5)

            origin = (s + jnp.where(b == 1, sp - 1, jnp.where(b == 2, 1, jnp.where(b == 3, 2, 0)))) % sp
        else:
            @pl.when(b == 1)
            def _():
                for step in range(1, sp):
                    source = lax.rem(s - step + sp, sp)
                    remote(kvs.at[source], kvs.at[source], zsend, zrecv, step - 1, "sp", source).wait_recv()

            origin = (s + b) % sp

        def q_rows(t, unused):
            if ring:
                @pl.when((b == 0) & (t == q_tiles - 1))
                def _():
                    forward(tiles - 2)

            at = pl.ds(pl.multiple_of(t * q_tile, q_tile), q_tile)
            for h in range(kv_heads):
                k = kvs[origin, 0, :, h * head : (h + 1) * head]
                v = kvs[origin, 1, :, h * head : (h + 1) * head]
                v_wide = jnp.concatenate([v, jnp.ones((keys, head), BF16)], axis=1)
                for g in range(group):
                    n = h * group + g
                    slot, lane = (n * head) // width, (n * head) % width
                    q = q_all[slot, at, lane : lane + head]
                    scores = lax.dot_general(q, k, (((1,), (1,)), ((), ())), preferred_element_type=F32)
                    scores = jnp.concatenate([scores[:, :lat_rows], scores[:, lat_rows:] + lift[n]], axis=1)
                    before = top[n, at, :]
                    now = jnp.maximum(before, jnp.max(scores, axis=-1, keepdims=True))
                    expo = jnp.exp(scores - now)
                    keep = jnp.exp(before - now)
                    top[n, at, :] = now
                    acc[n, at, :] = acc[n, at, :] * keep + jnp.dot(expo.astype(BF16), v_wide, preferred_element_type=F32)
            return unused

        lax.fori_loop(0, q_tiles, q_rows, 0)
        return unused

    lax.fori_loop(0, sp, block, 0)

    def close(t, unused):
        at = pl.ds(pl.multiple_of(t * q_tile, q_tile), q_tile)
        for pair in range(heads // 2):
            two = [acc[2 * pair + n, at, :] for n in range(2)]
            two = [v[:, :head] / v[:, head:] for v in two]
            attended[at, pair * 2 * head : (pair + 1) * 2 * head] = jnp.concatenate(two, axis=1).astype(BF16)
        return unused

    lax.fori_loop(0, q_tiles, close, 0)
    if ring:
        for number in range(tiles):
            for index in range(6):
                ring_copy(number, index).wait_send()
    else:
        for step in range(1, sp):
            direct(step).wait_send()
    for item in sends + outs:
        item.wait_send()
    gather.finish()


def back_kernel(tp, att, weight, out, full, wide, total, mixed, landed, send, recv, asend, arecv, local):
    f = lax.axis_index("tp")
    rows, cols = att.shape
    own_rows = out.shape[0]
    out_cols = weight.shape[1]
    load = pltpu.make_async_copy(weight, wide, local.at[0])
    load.start()
    mine = pltpu.make_async_copy(att, full.at[f], local.at[1])
    mine.start()
    greet(others("tp", tp))
    gather = Gather(tp, att, full, send, recv)
    gather.start()
    gather.second()
    total[...] = jnp.zeros(total.shape, F32)
    gather.relay()
    mine.wait()
    load.wait()
    r_tile = min(256, rows)

    def chip_step(index, unused):
        gather.before(index)
        chip = gather.chip(index)

        def row_step(t, unused):
            at = pl.ds(pl.multiple_of(t * r_tile, r_tile), r_tile)
            value = total[at, :]
            for n in range(2):
                source = chip * 2 + n
                depth = pl.ds(pl.multiple_of(source * cols, cols), cols)
                value = value + jnp.dot(full[source, at, :], wide[depth, :], preferred_element_type=F32)
            total[at, :] = value
            return unused

        lax.fori_loop(0, rows // r_tile, row_step, 0)
        return unused

    lax.fori_loop(0, tp // 2, chip_step, 0)
    for peer in range(tp):
        mixed[peer] = total[peer * own_rows : (peer + 1) * own_rows, :].astype(BF16)
    sends = []
    for step in range(1, tp):
        peer = lax.rem(f + step, tp)
        sends.append(remote(mixed.at[peer], landed.at[f], asend, arecv, step - 1, "tp", peer))
    for item in sends:
        item.start()
    landed[f] = mixed[f]
    for step in range(1, tp):
        origin = lax.rem(f - step + tp, tp)
        remote(landed.at[origin], landed.at[origin], asend, arecv, step - 1, "tp", origin).wait_recv()
    for n in range(tp):
        out[:, n * out_cols : (n + 1) * out_cols] = landed[n]
    for item in sends:
        item.wait_send()
    gather.finish()


def tables(first, count, head):
    freqs = head // 4
    lane = jnp.arange(2 * head, dtype=jnp.int32) % head
    inverse = 10000.0 ** (-(lane // 2 % freqs).astype(F32) / freqs)
    sign = jnp.where(lane % 2 == 0, -1.0, 1.0)
    grid_rows = -(-(count // GRID_W) // 8) * 8
    index = jnp.arange(grid_rows + GRID_W, dtype=jnp.int32)
    spot = jnp.where(index < grid_rows, index + first // GRID_W, index - grid_rows)
    angles = spot.astype(F32)[:, None] * inverse
    return jnp.cos(angles), jnp.sin(angles) * sign


def local(sp, tp, latent, context, condition, context_cond, mod_weight, norm_gain, query_weight, key_weight,
          value_weight, out_weight, query_gain, key_gain, context_lift):
    rows, model = latent.shape
    ctx_rows = context.shape[0]
    head = query_gain.shape[0]
    heads = query_weight.shape[1] // head
    kv_heads = key_weight.shape[1] // head
    width = key_weight.shape[1]
    slots = query_weight.shape[1] // width + 2
    block = rows * tp
    keys = block + ctx_rows
    limit = 60 * 1024 * 1024
    cond_pair = jax.nn.silu(jnp.stack([condition, context_cond])).astype(BF16)
    mcols = mod_weight.shape[1]
    cos, sin = tables(lax.axis_index("sp") * block, block, head)
    stacked = width % 128 != 0
    weights = [query_weight, key_weight, value_weight]
    if stacked:
        weights = [jnp.stack([query_weight[:, n * width : (n + 1) * width] for n in range(slots - 2)] + weights[1:])]
    dma = pltpu.SemaphoreType.DMA
    count = gather_sems(tp)
    pieces = (tp // 2 + 1) * 6 if sp == 4 else sp - 1
    attended, gate = pl.pallas_call(
        functools.partial(front_kernel, sp, tp, heads, kv_heads, head, stacked),
        name="front",
        out_shape=(jax.ShapeDtypeStruct((block, heads * head), BF16), jax.ShapeDtypeStruct((1, model), F32)),
        in_specs=[ANY, ANY, VMEM, ANY, VMEM, VMEM, VMEM, VMEM, VMEM, SMEM] + [ANY] * len(weights),
        out_specs=(VMEM, VMEM),
        scratch_shapes=[
            pltpu.VMEM((tp + 2, rows, model), BF16),
            pltpu.VMEM((2 * rows, model), BF16),
            pltpu.VMEM((slots, model, width), BF16),
            pltpu.VMEM(mod_weight.shape, BF16),
            pltpu.VMEM((sp, 2, mcols), F32),
            pltpu.VMEM((2, mcols), F32),
            pltpu.VMEM((2, mcols), F32),
            pltpu.VMEM((2, mcols * tp), F32),
            pltpu.VMEM((2, 1, model), F32),
            pltpu.VMEM((2, 1, model), F32),
            pltpu.VMEM((slots, 1, width), F32),
            pltpu.VMEM((slots - 2, block, width), BF16),
            pltpu.VMEM((sp, 2, keys, width), BF16),
            pltpu.VMEM((heads, block, 1), F32),
            pltpu.VMEM((heads, block, 2 * head), F32),
            dma((count,)), dma((count,)), dma((sp - 1,)), dma((sp - 1,)), dma((tp - 1,)), dma((tp - 1,)),
            dma((pieces,)), dma((pieces,)),
            dma((slots + 4,)),
        ],
        compiler_params=pltpu.CompilerParams(collective_id=0, has_side_effects=True, vmem_limit_bytes=limit),
    )(latent, context, cond_pair, mod_weight, norm_gain.reshape(1, model), cos, sin, query_gain.reshape(1, head),
      key_gain.reshape(1, head), context_lift, *weights)
    mixed = pl.pallas_call(
        functools.partial(back_kernel, tp),
        name="back",
        out_shape=jax.ShapeDtypeStruct((rows, model), BF16),
        in_specs=[VMEM, ANY],
        out_specs=VMEM,
        scratch_shapes=[
            pltpu.VMEM((tp, block, heads * head), BF16),
            pltpu.VMEM(out_weight.shape, BF16),
            pltpu.VMEM((block, out_weight.shape[1]), F32),
            pltpu.VMEM((tp, rows, out_weight.shape[1]), BF16),
            pltpu.VMEM((tp, rows, out_weight.shape[1]), BF16),
            dma((count,)), dma((count,)), dma((tp - 1,)), dma((tp - 1,)), dma((2,)),
        ],
        compiler_params=pltpu.CompilerParams(collective_id=2, has_side_effects=True, vmem_limit_bytes=limit),
    )(attended, out_weight)
    return (latent.astype(F32) + gate * mixed.astype(F32)).astype(BF16)


def solution(mesh):
    return jax.shard_map(
        functools.partial(local, mesh.shape["sp"], mesh.shape["tp"]),
        mesh=mesh,
        in_specs=(
            P(("sp", "tp"), None),
            P("sp", None),
            P("sp"),
            P("sp"),
            P("sp", "tp"),
            P(),
            P(None, "tp"),
            P(None, "tp"),
            P(None, "tp"),
            P(None, "tp"),
            P(),
            P(),
            P("tp"),
        ),
        out_specs=P(("sp", "tp"), None),
        check_vma=False,
    )
```
